32 devices in a mesh: ep: 8 (over z, x), tp: 4 (over y, core).
Axes of the slice: x: 2, y: 2, z: 4, core: 2. Of those that a mesh axis runs over, the one named last changes fastest.
Arguments:
- residual_in: bfloat16 [128, 2048], P('ep'), may hold values from -6 to 6
- lengths: int32 [128], P('ep'), may hold values from 1 to 511, as said below
- kv_cache: bfloat16 [128, 4, 512, 256], P('ep', 'tp'), may hold values from -640 to 640
- norm_gain_attn: float32 [2048], replicated, may hold values from 0.1 to 1.9
- query_weight: bfloat16 [2048, 2048], P(None, 'tp'), may hold values from -0.125 to 0.125
- key_weight: bfloat16 [2048, 512], P(None, 'tp'), may hold values from -0.125 to 0.125
- value_weight: bfloat16 [2048, 512], P(None, 'tp'), may hold values from -0.125 to 0.125
- diff_lambda: float32 [16], P('tp'), may hold values from 0.3 to 0.8
- head_gain: float32 [128], replicated, may hold values from 0.1 to 1.9
- out_weight: bfloat16 [2048, 2048], P(None, 'tp'), may hold values from -0.125 to 0.125
- norm_gain_ffn: float32 [2048], replicated, may hold values from 0.1 to 1.9
- route_ids: int32 [128, 2], P('ep'), may hold values from 0 to 7, as said below
- route_weights: float32 [128, 2], P('ep'), may hold values from 0.1 to 1
- expert_gate: bfloat16 [8, 2048, 512], P('ep', None, 'tp'), may hold values from -0.125 to 0.125
- expert_up: bfloat16 [8, 2048, 512], P('ep', None, 'tp'), may hold values from -0.125 to 0.125
- expert_down: bfloat16 [8, 512, 2048], P('ep', 'tp'), may hold values from -0.25 to 0.25
- dense_gate: bfloat16 [2048, 8192], P(None, 'ep'), may hold values from -0.125 to 0.125
- dense_up: bfloat16 [2048, 8192], P(None, 'ep'), may hold values from -0.125 to 0.125
- dense_down: bfloat16 [8192, 2048], P('ep'), may hold values from -0.0625 to 0.0625
- dense_mix: float32 [2048], replicated, may hold values from -0.125 to 0.125
Outputs:
- layer_out: bfloat16 [128, 2048], P('ep', 'tp')
- new_rows: bfloat16 [128, 4, 256], P('ep', 'tp')
The draws below stay inside these ranges and needn't reach their ends.
Inputs may be any that keep to these rules, and one draw needn't show every extreme that they name: The new token stands at position lengths[b]; some sequence holds 511 positions in every draw. `route_ids`: each row names 2 different experts from one group; the groups are the 4 runs of consecutive expert numbers of equal size. Among the rows of one index of ep no expert is named more than 8 times, and some expert exactly 8 times.
All inputs are finite; a program needn't handle non-finite values.
Results may differ from the reference program's by a relative error of at most 0.008.
The reference program's roundings to bfloat16 on the way count: a program that leaves them out, or rounds other values in their place, can miss the bound.
Values may be sent and summed in bfloat16 or wider, within the bound.
A program may use at most 64 MiB of HBM per device.

```python
import math
import jax
import jax.numpy as jnp
from jax import lax

D = 2048
HEADS = 16
KV_HEADS = 4
QK_DIM = 64
HEAD_DIM = 128
KV_WIDTH = 256
SEQ_DEV = 16
CACHE = 512
TOKENS = 128
EXPERTS = 8
GROUPS = 4
TOPK = 2
EXP_FF = 512
DENSE_FF = 8192
CAP = 8
N_EP = 8
N_TP = 4


def draw_lengths(key, part):
    raw = jax.random.randint(jax.random.fold_in(key, 21), (TOKENS,), 0, CACHE - 1)
    factor = jax.random.randint(jax.random.fold_in(key, 22), (TOKENS // SEQ_DEV, 1), 1, 9)
    spread = jnp.broadcast_to(factor, (TOKENS // SEQ_DEV, SEQ_DEV)).reshape(TOKENS)
    counts = 1 + raw * spread // 8
    longest = jax.random.randint(jax.random.fold_in(key, 23), (), 0, TOKENS)
    return jnp.where(jnp.arange(TOKENS, dtype=jnp.int32) == longest, CACHE - 1, counts).astype(jnp.int32)


def draw_kv_cache(key, part):
    base = jnp.clip(jax.random.normal(key, (TOKENS, KV_HEADS, CACHE, KV_WIDTH), jnp.float32), -6.0, 6.0)
    lane = lax.broadcasted_iota(jnp.int32, (1, 1, 1, KV_WIDTH), 3)
    level = jnp.ones((TOKENS, KV_HEADS, 1, 1), jnp.float32)
    factor = jnp.where(lane < 2 * QK_DIM, 1.75 * level, 1.0)
    return (base * factor).astype(jnp.bfloat16)


def draw_route_ids(key, part):
    blocks = TOKENS // SEQ_DEV
    per_group = EXPERTS // GROUPS
    busy_rows = CAP * per_group // TOPK
    busy = jax.random.randint(jax.random.fold_in(key, 41), (blocks, 1), 0, GROUPS)
    other = (busy + jax.random.randint(jax.random.fold_in(key, 42), (blocks, SEQ_DEV), 1, GROUPS)) % GROUPS
    place = lax.broadcasted_iota(jnp.int32, (blocks, SEQ_DEV), 1)
    ordered = jnp.where(place < busy_rows, busy, other)
    scores = jax.random.randint(jax.random.fold_in(key, 43), (blocks, SEQ_DEV), 0, 1 << 20) * SEQ_DEV + place
    order = jnp.argsort(scores, axis=1)
    group = jnp.take_along_axis(ordered, order, axis=1)
    member = (group[:, :, None] == jnp.arange(GROUPS, dtype=jnp.int32)[None, None, :]).astype(jnp.int32)
    rank = jnp.sum((jnp.cumsum(member, axis=1) - member) * member, axis=2)
    shift = TOPK * jax.random.randint(jax.random.fold_in(key, 44), (blocks, GROUPS), 0, per_group // TOPK)
    offset = jnp.take_along_axis(shift, group, axis=1)
    first = TOPK * rank + offset
    picks = [group * per_group + (first + step) % per_group for step in range(TOPK)]
    return jnp.stack(picks, axis=-1).reshape(TOKENS, TOPK).astype(jnp.int32)


def level_of(key, shape, shards, low, largest):
    def one(position, shards_of):
        steps = jax.random.uniform(jax.random.fold_in(jax.random.fold_in(key, 6), position), (shards_of,), jnp.float32, low / len(shards), largest / len(shards))
        return jnp.repeat(jnp.exp(steps), shape[position] // shards_of).reshape((-1,) + (1,) * (len(shape) - position - 1))

    level = one(*shards[0])
    for cut in shards[1:]:
        level = level * one(*cut)
    return level


def scatter_about(own_key, dims, scale, most, split=(), kind=jnp.bfloat16):
    level = level_of(own_key, dims, split, -0.22, 0.18) if split else 1.0
    array = jax.random.normal(own_key, dims, jnp.float32) * scale * level
    return jnp.minimum(jnp.maximum(array, -most), most).astype(kind)


def setup_inputs(seed: int = 0) -> dict:
    seeds = jax.random.split(jax.random.key(seed), 21)
    return {
        "residual_in": scatter_about(seeds[0], (TOKENS, D), 1.0, 6.0, ((0, 8),)),
        "lengths": draw_lengths(jax.random.fold_in(seeds[20], 71), 0),
        "kv_cache": draw_kv_cache(jax.random.fold_in(seeds[20], 71), 0),
        "norm_gain_attn": jnp.clip(1.0 + 0.18 * jax.random.normal(seeds[3], (D,), jnp.float32), 0.1, 1.9),
        "query_weight": scatter_about(seeds[4], (D, HEADS * 2 * QK_DIM), D ** -0.5, 0.125, ((1, 4),)),
        "key_weight": scatter_about(seeds[5], (D, KV_HEADS * 2 * QK_DIM), D ** -0.5, 0.125, ((1, 4),)),
        "value_weight": scatter_about(seeds[6], (D, KV_HEADS * HEAD_DIM), D ** -0.5, 0.125, ((1, 4),)),
        "diff_lambda": jnp.clip(0.3 + 0.5 * jax.random.uniform(seeds[7], (HEADS,), jnp.float32) ** level_of(seeds[7], (HEADS,), ((0, 4),), -0.2, 0.2), 0.3, 0.8),
        "head_gain": jnp.clip(1.0 + 0.18 * jax.random.normal(seeds[8], (HEAD_DIM,), jnp.float32), 0.1, 1.9),
        "out_weight": scatter_about(seeds[9], (HEADS * HEAD_DIM, D), (HEADS * HEAD_DIM) ** -0.5, 0.125, ((1, 4),)),
        "norm_gain_ffn": jnp.clip(1.0 + 0.18 * jax.random.normal(seeds[10], (D,), jnp.float32), 0.1, 1.9),
        "route_ids": draw_route_ids(jax.random.fold_in(seeds[20], 71), 0),
        "route_weights": jnp.clip(jnp.exp(math.log(1.0) - 2.3025851 * jax.random.uniform(seeds[12], (TOKENS, TOPK), jnp.float32) ** level_of(seeds[12], (TOKENS, TOPK), ((0, 8),), -0.2, 0.2)), 0.1, 1.0),
        "expert_gate": scatter_about(seeds[13], (EXPERTS, D, EXP_FF), D ** -0.5, 0.125, ((0, 8), (2, 4))),
        "expert_up": scatter_about(seeds[14], (EXPERTS, D, EXP_FF), D ** -0.5, 0.125, ((0, 8), (2, 4))),
        "expert_down": scatter_about(seeds[15], (EXPERTS, EXP_FF, D), EXP_FF ** -0.5, 0.25, ((0, 8), (1, 4))),
        "dense_gate": scatter_about(seeds[16], (D, DENSE_FF), D ** -0.5, 0.125, ((1, 8),)),
        "dense_up": scatter_about(seeds[17], (D, DENSE_FF), D ** -0.5, 0.125, ((1, 8),)),
        "dense_down": scatter_about(seeds[18], (DENSE_FF, D), DENSE_FF ** -0.5, 0.0625, ((0, 8),)),
        "dense_mix": scatter_about(seeds[19], (D,), D ** -0.5, 0.125, (), jnp.float32),
    }


EPS = 1e-06

def rms_rows(values, gain):
    mean_sq = lax.optimization_barrier(jnp.mean(values * values, axis=-1, keepdims=True))
    return values * lax.rsqrt(mean_sq + EPS) * gain

def rotate(vectors, positions):
    half = vectors.shape[-1] // 2
    inverse = 10000.0 ** (-jnp.arange(half, dtype=jnp.float32) / half)
    angle = positions[:, None, None, None] * inverse
    cosine = jnp.cos(angle)
    sine = jnp.sin(angle)
    first = vectors[..., :half]
    second = vectors[..., half:]
    return jnp.concatenate([first * cosine - second * sine, first * sine + second * cosine], axis=-1)

def normalize(scores, latest, valid):
    masked = jnp.where(valid, scores, -jnp.inf)
    top = jnp.maximum(lax.optimization_barrier(jnp.max(masked, axis=-1)), latest)
    raised = jnp.where(valid, jnp.exp(jnp.where(valid, scores, 0.0) - top[..., None]), 0.0)
    raised_new = jnp.exp(latest - top)
    total = lax.optimization_barrier(jnp.sum(raised, axis=-1)) + raised_new
    return (raised / total[..., None], raised_new / total)

def attend(query, fresh, cache, lengths, lam):
    count = fresh.shape[0]
    groups = fresh.shape[1]
    share = query.shape[1] // groups
    scale = QK_DIM ** (-0.5)
    grouped = query.astype(jnp.float32).reshape(count, groups, share, 2, QK_DIM)
    latest = fresh.astype(jnp.float32)
    stored = cache.astype(jnp.float32)
    first = jnp.einsum('bgjd,bgkd->bgjk', grouped[:, :, :, 0], stored[..., :QK_DIM]) * scale
    second = jnp.einsum('bgjd,bgkd->bgjk', grouped[:, :, :, 1], stored[..., QK_DIM:2 * QK_DIM]) * scale
    first_new = jnp.einsum('bgjd,bgd->bgj', grouped[:, :, :, 0], latest[..., :QK_DIM]) * scale
    second_new = jnp.einsum('bgjd,bgd->bgj', grouped[:, :, :, 1], latest[..., QK_DIM:2 * QK_DIM]) * scale
    valid = jnp.arange(cache.shape[2], dtype=jnp.int32)[None, None, None, :] < lengths[:, None, None, None]
    prob_one, prob_one_new = normalize(first, first_new, valid)
    prob_two, prob_two_new = normalize(second, second_new, valid)
    weight = lam.reshape(groups, share)[None, :, :, None]
    mapped = (prob_one - weight * prob_two).astype(jnp.bfloat16)
    mapped_new = (prob_one_new - weight[..., 0] * prob_two_new).astype(jnp.bfloat16)
    output = jnp.einsum('bgjk,bgkd->bgjd', mapped.astype(jnp.float32), stored[..., 2 * QK_DIM:])
    output = output + mapped_new.astype(jnp.float32)[..., None] * latest[:, :, None, 2 * QK_DIM:]
    return output.reshape(count, groups * share, HEAD_DIM)

def reference(residual_in, lengths, kv_cache, norm_gain_attn, query_weight, key_weight, value_weight, diff_lambda, head_gain, out_weight, norm_gain_ffn, route_ids, route_weights, expert_gate, expert_up, expert_down, dense_gate, dense_up, dense_down, dense_mix):
    blocks = TOKENS // SEQ_DEV
    resid = residual_in.astype(jnp.float32)
    normed = rms_rows(resid, norm_gain_attn).astype(jnp.bfloat16)
    positions = lengths.astype(jnp.float32)
    query = jnp.dot(normed, query_weight, preferred_element_type=jnp.float32).reshape(TOKENS, HEADS, 2, QK_DIM)
    query = rotate(query, positions).astype(jnp.bfloat16)
    keys = jnp.dot(normed, key_weight, preferred_element_type=jnp.float32).reshape(TOKENS, KV_HEADS, 2, QK_DIM)
    keys = rotate(keys, positions).astype(jnp.bfloat16).reshape(TOKENS, KV_HEADS, 2 * QK_DIM)
    values = jnp.dot(normed, value_weight, preferred_element_type=jnp.float32).reshape(TOKENS, KV_HEADS, HEAD_DIM).astype(jnp.bfloat16)
    fresh = jnp.concatenate([keys, values], axis=-1)

    def per_block(items):
        return attend(items[0], items[1], items[2], items[3], diff_lambda)
    mixed = lax.map(per_block, (query.reshape(blocks, SEQ_DEV, HEADS, 2, QK_DIM), fresh.reshape(blocks, SEQ_DEV, KV_HEADS, KV_WIDTH), kv_cache.reshape(blocks, SEQ_DEV, KV_HEADS, CACHE, KV_WIDTH), lengths.reshape(blocks, SEQ_DEV)))
    mixed = mixed.reshape(TOKENS, HEADS, HEAD_DIM)
    heads_out = rms_rows(mixed, head_gain).astype(jnp.bfloat16).reshape(TOKENS, HEADS * HEAD_DIM)
    stream = (resid + jnp.dot(heads_out, out_weight, preferred_element_type=jnp.float32)).astype(jnp.bfloat16)
    ffn_in = rms_rows(stream.astype(jnp.float32), norm_gain_ffn).astype(jnp.bfloat16)
    flat_ids = route_ids.reshape(blocks, SEQ_DEV * TOPK)
    member = (flat_ids[..., None] == jnp.arange(EXPERTS, dtype=jnp.int32)[None, None, :]).astype(jnp.int32)
    slot = lax.optimization_barrier(jnp.sum((jnp.cumsum(member, axis=1) - member) * member, axis=2))
    block_of = lax.broadcasted_iota(jnp.int32, (blocks, SEQ_DEV * TOPK), 0)
    place = (flat_ids * N_EP + block_of) * CAP + slot
    owner = block_of * SEQ_DEV + lax.broadcasted_iota(jnp.int32, (blocks, SEQ_DEV * TOPK), 1) // TOPK
    table = jnp.zeros((EXPERTS * N_EP * CAP,), jnp.int32).at[place.reshape(-1)].set(owner.reshape(-1))
    quarter = EXP_FF // N_TP

    def expert_rows(items):
        index, w_gate, w_up, w_down = items
        chosen = ffn_in[index]
        gate = jnp.dot(chosen, w_gate, preferred_element_type=jnp.float32)
        upward = jnp.dot(chosen, w_up, preferred_element_type=jnp.float32)
        hidden = (jax.nn.silu(gate) * upward).astype(jnp.bfloat16)
        total = jnp.zeros((chosen.shape[0], D), jnp.float32)
        for part in range(N_TP):
            piece = jnp.dot(hidden[:, part * quarter:(part + 1) * quarter], w_down[part * quarter:(part + 1) * quarter], preferred_element_type=jnp.float32).astype(jnp.bfloat16)
            total = total + lax.optimization_barrier(piece).astype(jnp.float32)
        return total.astype(jnp.bfloat16)
    results = lax.map(expert_rows, (table.reshape(EXPERTS, N_EP * CAP), expert_gate, expert_up, expert_down))
    flat_results = results.reshape(EXPERTS * N_EP * CAP, D)
    picked = flat_results[place.reshape(TOKENS, TOPK)]
    moe = lax.optimization_barrier(jnp.sum(route_weights[..., None] * picked.astype(jnp.float32), axis=1))
    dense_g = jnp.dot(ffn_in, dense_gate, preferred_element_type=jnp.float32)
    dense_u = jnp.dot(ffn_in, dense_up, preferred_element_type=jnp.float32)
    dense_hidden = (jax.nn.silu(dense_g) * dense_u).astype(jnp.bfloat16)
    dense = jnp.dot(dense_hidden, dense_down, preferred_element_type=jnp.float32)
    mix = jax.nn.sigmoid(lax.optimization_barrier(jnp.sum(ffn_in.astype(jnp.float32) * dense_mix, axis=-1)))
    layer_out = (stream.astype(jnp.float32) + moe + mix[:, None] * dense).astype(jnp.bfloat16)
    return (layer_out, fresh)
```

```python
import functools

import jax
import jax.numpy as jnp
from jax import lax
from jax.experimental import pallas as pl
from jax.experimental.pallas import tpu as pltpu
from jax.sharding import PartitionSpec as P

QK_DIM = 64
HEAD_DIM = 128


EPS = 1e-06


def rms_rows(values, gain):
    mean_sq = jnp.mean(values * values, axis=-1, keepdims=True)
    return values * lax.rsqrt(mean_sq + EPS) * gain


def rotate(vectors, positions):
    half = vectors.shape[-1] // 2
    inverse = 10000.0 ** (-jnp.arange(half, dtype=jnp.float32) / half)
    angle = positions[:, None, None, None] * inverse
    cosine = jnp.cos(angle)
    sine = jnp.sin(angle)
    first = vectors[..., :half]
    second = vectors[..., half:]
    return jnp.concatenate(
        [first * cosine - second * sine, first * sine + second * cosine], axis=-1
    )


def normalize(scores, latest, valid):
    masked = jnp.where(valid, scores, -jnp.inf)
    top = jnp.maximum(jnp.max(masked, axis=-1), latest)
    raised = jnp.where(valid, jnp.exp(jnp.where(valid, scores, 0.0) - top[..., None]), 0.0)
    raised_new = jnp.exp(latest - top)
    total = jnp.sum(raised, axis=-1) + raised_new
    return (raised / total[..., None], raised_new / total)


def attend(query, fresh, cache, lengths, lam):
    count = fresh.shape[0]
    groups = fresh.shape[1]
    share = query.shape[1] // groups
    scale = QK_DIM ** (-0.5)
    grouped = query.reshape(count, groups, share, 2, QK_DIM)
    first = (
        jnp.einsum(
            "bgjd,bgkd->bgjk",
            grouped[:, :, :, 0],
            cache[..., :QK_DIM],
            preferred_element_type=jnp.float32,
        )
        * scale
    )
    second = (
        jnp.einsum(
            "bgjd,bgkd->bgjk",
            grouped[:, :, :, 1],
            cache[..., QK_DIM : 2 * QK_DIM],
            preferred_element_type=jnp.float32,
        )
        * scale
    )
    first_new = (
        jnp.einsum(
            "bgjd,bgd->bgj",
            grouped[:, :, :, 0],
            fresh[..., :QK_DIM],
            preferred_element_type=jnp.float32,
        )
        * scale
    )
    second_new = (
        jnp.einsum(
            "bgjd,bgd->bgj",
            grouped[:, :, :, 1],
            fresh[..., QK_DIM : 2 * QK_DIM],
            preferred_element_type=jnp.float32,
        )
        * scale
    )
    valid = (
        jnp.arange(cache.shape[2], dtype=jnp.int32)[None, None, None, :]
        < lengths[:, None, None, None]
    )
    prob_one, prob_one_new = normalize(first, first_new, valid)
    prob_two, prob_two_new = normalize(second, second_new, valid)
    weight = lam.reshape(groups, share)[None, :, :, None]
    mapped = (prob_one - weight * prob_two).astype(jnp.bfloat16)
    mapped_new = (prob_one_new - weight[..., 0] * prob_two_new).astype(jnp.bfloat16)
    output = jnp.einsum(
        "bgjk,bgkd->bgjd", mapped, cache[..., 2 * QK_DIM :], preferred_element_type=jnp.float32
    )
    output = output + mapped_new.astype(jnp.float32)[..., None] * fresh[
        :, :, None, 2 * QK_DIM :
    ].astype(jnp.float32)
    return output.reshape(count, groups * share, HEAD_DIM)


MESH = pl.DeviceIdType.MESH
F32 = jnp.float32
BF16 = jnp.bfloat16
LANES = 128


def flip(value, mask):
    bit = 1
    while bit <= mask:
        if mask & bit:
            value = value + bit * (1 - 2 * ((value // bit) % 2))
        bit *= 2
    return value


def each(count, body, order=None):
    if count <= 16:
        for index in order if order is not None else range(count):
            body(index)
    else:

        def step(index, carry):
            body(index)
            return carry

        lax.fori_loop(0, count, step, 0)


def block(start, size):
    return pl.ds(pl.multiple_of(start * size, size), size)


def remote(source, target, send, recv, where):
    return pltpu.make_async_remote_copy(
        src_ref=source,
        dst_ref=target,
        send_sem=send,
        recv_sem=recv,
        device_id=where,
        device_id_type=MESH,
    )


def dot(left, right):
    return jnp.dot(left, right, preferred_element_type=F32)


def layer_kernel(
    n_ep,
    n_tp,
    split,
    heads_ref,
    resid_ref,
    gain_ref,
    mixw_ref,
    ids_ref,
    rw_ref,
    ow_hbm,
    eg_hbm,
    eu_hbm,
    ed_hbm,
    dg_hbm,
    du_hbm,
    dd_hbm,
    out_ref,
    ow,
    eg,
    eu,
    ed,
    dg,
    du,
    dd,
    heads_all,
    stream,
    ffn,
    mix,
    route,
    eh,
    dh,
    away,
    came,
    summed,
    landed,
    w_sem,
    route_send,
    route_recv,
    heads_send,
    heads_recv,
    first_send,
    second_send,
    relay_send,
    stream_recv,
    pair_send,
    pair_recv,
    back_send,
    back_recv,
):
    e = lax.axis_index("ep")
    t = lax.axis_index("tp")
    half = n_tp // 2
    mate = flip(t, 1)
    core = t % 2
    seqs, width = resid_ref.shape
    quarter = out_ref.shape[1]
    held, _, part = eg.shape
    hid = dg.shape[1]
    rows_all = n_ep * seqs
    evens = [2 * i for i in range(1, half)]

    barrier = pltpu.get_barrier_semaphore()

    def greet(index):
        where = (index // half, 2 * (index % half) + core)

        @pl.when(jnp.logical_or(where[0] != e, where[1] != t))
        def _():
            pl.semaphore_signal(barrier, inc=1, device_id=where, device_id_type=MESH)

    each(n_ep * half, greet)
    for i in range(half):
        pl.semaphore_signal(
            barrier, inc=1, device_id=(e, 2 * i + 1 - core), device_id_type=MESH
        )

    if split:
        cols = block(t, hid)
        dense_parts = (dg_hbm.at[:, cols], du_hbm.at[:, cols], dd_hbm.at[cols, :])
    else:
        dense_parts = (dg_hbm, du_hbm, dd_hbm)
    loads = [
        pltpu.make_async_copy(src, dst, w_sem.at[i])
        for i, (src, dst) in enumerate(
            zip((ow_hbm, eg_hbm, eu_hbm) + dense_parts[:2] + (ed_hbm, dense_parts[2]), (ow, eg, eu, dg, du, ed, dd))
        )
    ]
    for load in loads:
        load.start()

    lane = lax.broadcasted_iota(jnp.int32, (seqs, route.shape[1]), 1)
    table = jnp.zeros((seqs, route.shape[1]), F32)
    for k in range(ids_ref.shape[1]):
        table = table + jnp.where(lane == ids_ref[:, k : k + 1], rw_ref[:, k : k + 1], 0.0)
    own_rows = block(e, seqs)
    route[own_rows, :] = table

    pl.semaphore_wait(barrier, n_ep * half - 1 + half)

    def heads_copy(mask):
        return remote(
            heads_ref,
            heads_all.at[mask - 1],
            heads_send.at[mask - 1],
            heads_recv.at[mask - 1],
            (e, flip(t, mask)),
        )

    for mask in range(n_tp - 1, 0, -1):
        heads_copy(mask).start()

    def route_copy(d):
        there = (e + d) % n_ep
        return remote(
            route.at[own_rows, :],
            route.at[own_rows, :],
            route_send.at[d - 1],
            route_recv.at[d - 1],
            (there, t),
        )

    def route_wait(d):
        came_from = (e + n_ep - d) % n_ep
        spot = route.at[block(came_from, seqs), :]
        remote(spot, spot, route_send.at[d - 1], route_recv.at[d - 1], (e, t)).wait_recv()

    each(n_ep - 1, lambda i: route_copy(i + 1).start())

    loads[0].wait()
    span = heads_ref.shape[1]
    total = dot(heads_ref[...], ow[block(t, span), :])
    for mask in range(1, n_tp):
        heads_copy(mask).wait_recv()
        total = total + dot(heads_all[mask - 1], ow[block(flip(t, mask), span), :])
    own_cols = block(t, quarter)
    own_stream = (resid_ref[:, own_cols].astype(F32) + total).astype(BF16)
    stream[own_rows, own_cols] = own_stream

    def spot(owner, column):
        return stream.at[block(owner, seqs), block(column, quarter)]

    def owner_of(d):
        return (e + n_ep - d) % n_ep

    def first(d):
        return remote(
            spot(e, t), spot(e, t), first_send.at[d], stream_recv.at[0, d], ((e + d) % n_ep, t)
        )

    def second(d, mask):
        index = mask // 2 if mask != 1 else 0
        where = spot(owner_of(d), t)
        return remote(
            where, where, second_send.at[index, d], stream_recv.at[mask, d], (e, flip(t, mask))
        )

    def relay(d, mask):
        where = spot(owner_of(d), flip(t, mask))
        return remote(
            where, where, relay_send.at[mask // 2 - 1, d], stream_recv.at[mask + 1, d], (e, mate)
        )

    def arrived(d, mask):
        where = spot(owner_of(d), flip(t, mask))
        remote(where, where, first_send.at[d], stream_recv.at[mask, d], (e, t)).wait_recv()

    def spread(d):
        for mask in evens:
            second(d, mask).start()
        second(d, 1).start()

    far_first = sorted(range(1, n_ep), key=lambda d: -min(d, n_ep - d)) if n_ep <= 16 else None
    near_first = [0] + far_first[::-1] if far_first is not None else None
    each(n_ep - 1 if far_first is None else 1, lambda i: first(i + 1).start(), order=None) if far_first is None else [
        first(d).start() for d in far_first
    ]

    def stage_two(d):
        if not (isinstance(d, int) and d == 0):
            arrived(d, 0)
        spread(d)

    def stage_three(d):
        for mask in evens:
            arrived(d, mask)
            relay(d, mask).start()

    def normalise(d):
        arrived(d, 1)
        for mask in evens:
            arrived(d, mask + 1)
        rows = block(owner_of(d), seqs)
        values = stream[rows, :].astype(F32)
        mean_sq = jnp.mean(values * values, axis=-1, keepdims=True)
        scaled = (values * lax.rsqrt(mean_sq + EPS) * gain_ref[...]).astype(BF16)
        ffn[rows, :] = scaled
        inner = jnp.sum(scaled.astype(F32) * mixw_ref[...], axis=-1, keepdims=True)
        mix[rows, :] = jnp.broadcast_to(jax.nn.sigmoid(inner), (seqs, LANES))

    if near_first is not None:
        for i, d in enumerate(near_first):
            stage_two(d)
            if i:
                stage_three(near_first[i - 1])
            if i > 1:
                normalise(near_first[i - 2])
        stage_three(near_first[-1])
        for d in near_first[-2:]:
            normalise(d)
    else:
        stage_two(0)
        each(n_ep - 1, lambda i: stage_two(i + 1))
        each(n_ep, stage_three)
        each(n_ep, normalise)
    each(n_ep - 1, lambda i: route_wait(i + 1))

    many = min(rows_all, 128)
    batches = rows_all // many
    for load in loads[1:5]:
        load.wait()

    def hidden(b):
        rows = block(b, many)
        a = ffn[rows, :]
        for j in range(held):
            eh[j, rows, :] = (jax.nn.silu(dot(a, eg[j])) * dot(a, eu[j])).astype(BF16)
        units = jax.nn.silu(dot(a, dg[...])) * dot(a, du[...])
        if not split:
            own = hid // n_tp
            unit = lax.broadcasted_iota(jnp.int32, units.shape, 1)
            units = jnp.where((unit >= t * own) & (unit < (t + 1) * own), units, 0.0)
        dh[rows, :] = units.astype(BF16)

    each(batches, hidden)
    for load in loads[5:]:
        load.wait()

    def result(b, q):
        rows = block(b, many)
        cols = block(q, quarter)
        total = mix[rows, :1] * dot(dh[rows, :], dd[:, cols])
        lanes = lax.broadcasted_iota(jnp.int32, (many, route.shape[1]), 1)
        for j in range(held):
            weight = jnp.sum(
                jnp.where(lanes == e * held + j, route[rows, :], 0.0), axis=1, keepdims=True
            )
            piece = dot(eh[j, rows, :], ed[j, :, cols]).astype(BF16)
            total = total + weight * piece.astype(F32)
        return total

    def pair(j):
        return remote(away.at[j], came.at[j], pair_send.at[j], pair_recv.at[j], (e, mate))

    for j in range(half):

        def leave(b, j=j):
            away[j, block(b, many), :] = result(b, 2 * j + 1 - core).astype(BF16)

        each(batches, leave)
        pair(j).start()

    me = e * half + t // 2

    def back(j, d):
        there = (e + d) % n_ep
        return remote(
            summed.at[j, block(there, seqs), :],
            landed.at[me],
            back_send.at[j, d],
            back_recv.at[me],
            (there, 2 * j + core),
        )

    def same(j, d):
        return jnp.logical_and(jnp.asarray(d == 0), 2 * j + core == t)

    for j in range(half):

        def keep(b, j=j):
            summed[j, block(b, many), :] = result(b, 2 * j + core).astype(BF16)

        each(batches, keep)
    for j in range(half):
        pair(j).wait_recv()

        def add(b, j=j):
            rows = block(b, many)
            summed[j, rows, :] = (summed[j, rows, :].astype(F32) + came[j, rows, :].astype(F32)).astype(BF16)

        each(batches, add)

        def send(d, j=j):
            @pl.when(jnp.logical_not(same(j, d)))
            def _():
                back(j, d).start()

        each(n_ep, send, order=None if far_first is None else far_first + [0])

    landed[me] = summed[t // 2, own_rows, :]

    def take(index):
        @pl.when(index != me)
        def _():
            where = landed.at[index]
            remote(where, where, back_send.at[0, 0], back_recv.at[index], (e, t)).wait_recv()

    each(n_ep * half, take)
    out_ref[...] = (
        own_stream.astype(F32) + jnp.sum(landed[...].astype(F32), axis=0)
    ).astype(BF16)

    for mask in range(1, n_tp):
        heads_copy(mask).wait_send()
    each(n_ep - 1, lambda i: route_copy(i + 1).wait_send())
    each(n_ep - 1, lambda i: first(i + 1).wait_send())

    def sent(d):
        second(d, 1).wait_send()
        for mask in evens:
            second(d, mask).wait_send()
            relay(d, mask).wait_send()

    each(n_ep, sent)
    for j in range(half):
        pair(j).wait_send()

        def gone(d, j=j):
            @pl.when(jnp.logical_not(same(j, d)))
            def _():
                back(j, d).wait_send()

        each(n_ep, gone)


def layer_call(heads, resid, gain, mixw, ids, rw, ow, eg, eu, ed, dg, du, dd):
    n_ep = lax.axis_size("ep")
    n_tp = lax.axis_size("tp")
    half = n_tp // 2
    seqs, width = resid.shape
    quarter = ow.shape[1]
    held, _, part = eg.shape
    rows = n_ep * seqs
    own = dg.shape[1] // n_tp
    split = own % LANES == 0
    hid = own if split else dg.shape[1]
    lanes = -(-n_ep * held // LANES) * LANES
    vmem = pl.BlockSpec(memory_space=pltpu.VMEM)
    hbm = pl.BlockSpec(memory_space=pl.ANY)
    dma = pltpu.SemaphoreType.DMA
    return pl.pallas_call(
        functools.partial(layer_kernel, n_ep, n_tp, split),
        out_shape=jax.ShapeDtypeStruct((seqs, quarter), BF16),
        in_specs=[vmem] * 6 + [hbm] * 7,
        out_specs=vmem,
        scratch_shapes=[
            pltpu.VMEM(ow.shape, BF16),
            pltpu.VMEM(eg.shape, BF16),
            pltpu.VMEM(eu.shape, BF16),
            pltpu.VMEM(ed.shape, BF16),
            pltpu.VMEM((width, hid), BF16),
            pltpu.VMEM((width, hid), BF16),
            pltpu.VMEM((hid, width), BF16),
            pltpu.VMEM((n_tp - 1,) + heads.shape, BF16),
            pltpu.VMEM((rows, width), BF16),
            pltpu.VMEM((rows, width), BF16),
            pltpu.VMEM((rows, LANES), F32),
            pltpu.VMEM((rows, lanes), F32),
            pltpu.VMEM((held, rows, part), BF16),
            pltpu.VMEM((rows, hid), BF16),
            pltpu.VMEM((half, rows, quarter), BF16),
            pltpu.VMEM((half, rows, quarter), BF16),
            pltpu.VMEM((half, rows, quarter), BF16),
            pltpu.VMEM((n_ep * half, seqs, quarter), BF16),
            dma((7,)),
            dma((n_ep - 1,)),
            dma((n_ep - 1,)),
            dma((n_tp - 1,)),
            dma((n_tp - 1,)),
            dma((n_ep,)),
            dma((half, n_ep)),
            dma((max(half - 1, 1), n_ep)),
            dma((n_tp, n_ep)),
            dma((half,)),
            dma((half,)),
            dma((half, n_ep)),
            dma((n_ep * half,)),
        ],
        compiler_params=pltpu.CompilerParams(
            collective_id=0, has_side_effects=True, vmem_limit_bytes=56 * 1024 * 1024
        ),
    )(heads, resid, gain, mixw, ids, rw, ow, eg, eu, ed, dg, du, dd)


def on_device(
    residual_in,
    lengths,
    kv_cache,
    norm_gain_attn,
    query_weight,
    key_weight,
    value_weight,
    diff_lambda,
    head_gain,
    out_weight,
    norm_gain_ffn,
    route_ids,
    route_weights,
    expert_gate,
    expert_up,
    expert_down,
    dense_gate,
    dense_up,
    dense_down,
    dense_mix,
):
    seq_count, width = residual_in.shape
    groups = kv_cache.shape[1]
    local_heads = diff_lambda.shape[0]
    resid = residual_in.astype(jnp.float32)
    normed = rms_rows(resid, norm_gain_attn).astype(jnp.bfloat16)
    positions = lengths.astype(jnp.float32)
    query = jnp.dot(normed, query_weight, preferred_element_type=jnp.float32).reshape(
        seq_count, local_heads, 2, QK_DIM
    )
    query = rotate(query, positions).astype(jnp.bfloat16)
    keys = jnp.dot(normed, key_weight, preferred_element_type=jnp.float32).reshape(
        seq_count, groups, 2, QK_DIM
    )
    keys = rotate(keys, positions).astype(jnp.bfloat16).reshape(seq_count, groups, 2 * QK_DIM)
    values = (
        jnp.dot(normed, value_weight, preferred_element_type=jnp.float32)
        .reshape(seq_count, groups, HEAD_DIM)
        .astype(jnp.bfloat16)
    )
    fresh = jnp.concatenate([keys, values], axis=-1)
    mixed = attend(query, fresh, kv_cache, lengths, diff_lambda)
    heads_out = (
        rms_rows(mixed, head_gain).astype(jnp.bfloat16).reshape(seq_count, local_heads * HEAD_DIM)
    )
    layer_out = layer_call(
        heads_out,
        residual_in,
        norm_gain_ffn[None, :],
        dense_mix[None, :],
        route_ids,
        route_weights,
        out_weight,
        expert_gate,
        expert_up,
        expert_down,
        dense_gate,
        dense_up,
        dense_down,
    )
    return (layer_out, fresh)


def solution(mesh):
    placed = (
        P("ep", None),
        P("ep"),
        P("ep", "tp", None, None),
        P(),
        P(None, "tp"),
        P(None, "tp"),
        P(None, "tp"),
        P("tp"),
        P(),
        P(None, "tp"),
        P(),
        P("ep", None),
        P("ep", None),
        P("ep", None, "tp"),
        P("ep", None, "tp"),
        P("ep", "tp", None),
        P(None, "ep"),
        P(None, "ep"),
        P("ep", None),
        P(),
    )
    return jax.shard_map(
        on_device,
        mesh=mesh,
        in_specs=placed,
        out_specs=(P("ep", "tp"), P("ep", "tp", None)),
        check_vma=False,
    )
```

```python
import functools
import math

import jax
import jax.numpy as jnp
from jax import lax
from jax.experimental import pallas as pl
from jax.experimental.pallas import tpu as pltpu
from jax.sharding import PartitionSpec as P

QK_DIM = 64
EPS = 1e-06
MESH = pl.DeviceIdType.MESH
F32 = jnp.float32
BF16 = jnp.bfloat16
LANES = 128
Q_CHUNKS = 4


def flip(value, mask):
    bit = 1
    while bit <= mask:
        if mask & bit:
            value = value + bit * (1 - 2 * ((value // bit) % 2))
        bit *= 2
    return value


def each(count, body, order=None):
    if count <= 16:
        for index in order if order is not None else range(count):
            body(index)
    else:

        def step(index, carry):
            body(index)
            return carry

        lax.fori_loop(0, count, step, 0)


def block(start, size):
    return pl.ds(pl.multiple_of(start * size, size), size)


def remote(source, target, send, recv, where):
    return pltpu.make_async_remote_copy(
        src_ref=source,
        dst_ref=target,
        send_sem=send,
        recv_sem=recv,
        device_id=where,
        device_id_type=MESH,
    )


def dot(left, right):
    return jnp.dot(left, right, preferred_element_type=F32)


def column(row):
    count = row.shape[1]
    square = (count, count)
    same = lax.broadcasted_iota(jnp.int32, square, 0) == lax.broadcasted_iota(jnp.int32, square, 1)
    return jnp.sum(jnp.where(same, row, jnp.zeros_like(row)), axis=1, keepdims=True)


def layer_kernel(
    n_ep,
    n_tp,
    split,
    lengths_ref,
    lam_ref,
    resid_ref,
    first_gain_ref,
    head_gain_ref,
    gain_ref,
    mixw_ref,
    ids_ref,
    rw_ref,
    qw_hbm,
    kw_hbm,
    vw_hbm,
    cache_hbm,
    ow_hbm,
    eg_hbm,
    eu_hbm,
    ed_hbm,
    dg_hbm,
    du_hbm,
    dd_hbm,
    out_ref,
    new_ref,
    qw,
    kw,
    vw,
    cache,
    pairs,
    scores,
    mixed,
    heads_ref,
    ow,
    eg,
    eu,
    ed,
    dg,
    du,
    dd,
    heads_all,
    stream,
    ffn,
    mix,
    route,
    eh,
    dh,
    away,
    came,
    summed,
    landed,
    w_sem,
    q_sem,
    cache_sem,
    route_send,
    route_recv,
    heads_send,
    heads_recv,
    first_send,
    second_send,
    relay_send,
    stream_recv,
    pair_send,
    pair_recv,
    back_send,
    back_recv,
):
    e = lax.axis_index("ep")
    t = lax.axis_index("tp")
    half = n_tp // 2
    mate = flip(t, 1)
    core = t % 2
    seqs, width = resid_ref.shape
    quarter = out_ref.shape[1]
    held, _, part = eg.shape
    hid = dg.shape[1]
    rows_all = n_ep * seqs
    evens = [2 * i for i in range(1, half)]

    depth = qw.shape[0] // Q_CHUNKS
    q_loads = [
        pltpu.make_async_copy(
            qw_hbm.at[pl.ds(i * depth, depth), :], qw.at[pl.ds(i * depth, depth), :], q_sem.at[i]
        )
        for i in range(Q_CHUNKS)
    ] + [
        pltpu.make_async_copy(kw_hbm, kw, q_sem.at[Q_CHUNKS]),
        pltpu.make_async_copy(vw_hbm, vw, q_sem.at[Q_CHUNKS + 1]),
    ]
    for load in q_loads:
        load.start()
    cache_loads = [
        pltpu.make_async_copy(cache_hbm.at[s], cache.at[s], cache_sem.at[s]) for s in range(seqs)
    ]
    for load in cache_loads:
        load.start()

    barrier = pltpu.get_barrier_semaphore()

    def greet(index):
        where = (index // half, 2 * (index % half) + core)

        @pl.when(jnp.logical_or(where[0] != e, where[1] != t))
        def _():
            pl.semaphore_signal(barrier, inc=1, device_id=where, device_id_type=MESH)

    each(n_ep * half, greet)
    for i in range(half):
        pl.semaphore_signal(
            barrier, inc=1, device_id=(e, 2 * i + 1 - core), device_id_type=MESH
        )

    if split:
        cols = block(t, hid)
        dense_parts = (dg_hbm.at[:, cols], du_hbm.at[:, cols], dd_hbm.at[cols, :])
    else:
        dense_parts = (dg_hbm, du_hbm, dd_hbm)
    loads = [
        pltpu.make_async_copy(src, dst, w_sem.at[i])
        for i, (src, dst) in enumerate(
            zip((ow_hbm, eg_hbm, eu_hbm) + dense_parts[:2] + (ed_hbm, dense_parts[2]), (ow, eg, eu, dg, du, ed, dd))
        )
    ]

    lane = lax.broadcasted_iota(jnp.int32, (seqs, route.shape[1]), 1)
    table = jnp.zeros((seqs, route.shape[1]), F32)
    for k in range(ids_ref.shape[0]):
        wanted = column(ids_ref[k : k + 1, :])
        table = table + jnp.where(lane == wanted, column(rw_ref[k : k + 1, :]), 0.0)
    own_rows = block(e, seqs)
    route[own_rows, :] = table

    resid = resid_ref[...].astype(F32)
    mean_sq = jnp.mean(resid * resid, axis=-1, keepdims=True)
    normed = (resid * lax.rsqrt(mean_sq + EPS) * first_gain_ref[...]).astype(BF16)
    row = lax.broadcasted_iota(jnp.int32, (seqs, LANES), 0)
    entry = lax.broadcasted_iota(jnp.int32, (seqs, LANES), 1) % QK_DIM
    position = jnp.zeros((seqs, LANES), F32)
    for s in range(seqs):
        position = jnp.where(row == s, lengths_ref[s].astype(F32), position)
    turn = QK_DIM // 2
    power = (entry % turn).astype(F32) * (-1.0 / turn)
    angle = position * jnp.exp(power * math.log(10000.0))
    cosine = jnp.cos(angle)
    sine = jnp.where(entry < turn, -jnp.sin(angle), jnp.sin(angle))

    def rotate(values):
        other = jnp.where(
            entry < turn, pltpu.roll(values, LANES - turn, 1), pltpu.roll(values, turn, 1)
        )
        return (values * cosine + other * sine).astype(BF16).astype(F32)

    query = jnp.zeros((seqs, qw.shape[1]), F32)
    for i in range(Q_CHUNKS):
        q_loads[i].wait()
        query = query + dot(
            normed[:, i * depth : (i + 1) * depth], qw[i * depth : (i + 1) * depth, :]
        )
    for load in q_loads[Q_CHUNKS:]:
        load.wait()
    keys_raw = dot(normed, kw[...])
    values_raw = dot(normed, vw[...])
    for load in loads:
        load.start()

    groups, spots = cache.shape[1], cache.shape[2]
    share = query.shape[1] // LANES // groups
    lower = lax.broadcasted_iota(jnp.int32, (seqs, LANES), 1) < QK_DIM
    fresh = []
    for g in range(groups):
        key = rotate(keys_raw[:, g * LANES : (g + 1) * LANES])
        value = values_raw[:, g * LANES : (g + 1) * LANES].astype(BF16).astype(F32)
        new_ref[:, 2 * g * LANES : (2 * g + 1) * LANES] = key
        new_ref[:, (2 * g + 1) * LANES : (2 * g + 2) * LANES] = value
        fresh.append((key, value))
        for j in range(share):
            at = (g * share + j) * LANES
            head = rotate(query[:, at : at + LANES])
            pairs[g, :, j, :] = jnp.where(lower, head, 0.0)
            pairs[g, :, share + j, :] = jnp.where(lower, 0.0, head)

    pl.semaphore_wait(barrier, n_ep * half - 1 + half)

    def route_copy(d):
        there = (e + d) % n_ep
        return remote(
            route.at[own_rows, :],
            route.at[own_rows, :],
            route_send.at[d - 1],
            route_recv.at[d - 1],
            (there, t),
        )

    def route_wait(d):
        came_from = (e + n_ep - d) % n_ep
        spot = route.at[block(came_from, seqs), :]
        remote(spot, spot, route_send.at[d - 1], route_recv.at[d - 1], (e, t)).wait_recv()

    each(n_ep - 1, lambda i: route_copy(i + 1).start())

    scale = QK_DIM**-0.5
    lines = 2 * share
    for s in range(seqs):
        cache_loads[s].wait()
        for g in range(groups):
            both = pairs[g, s].astype(BF16)
            scores[g, s] = (
                lax.dot_general(
                    both,
                    cache[s, g, :, :LANES],
                    (((1,), (1,)), ((), ())),
                    preferred_element_type=F32,
                )
                * scale
            )
    length = jnp.zeros((seqs, lines, 1), jnp.int32)
    which = lax.broadcasted_iota(jnp.int32, (seqs, lines, 1), 0)
    for s in range(seqs):
        length = jnp.where(which == s, lengths_ref[s], length)
    place = lax.broadcasted_iota(jnp.int32, (seqs, lines, spots), 2)
    valid = place < length
    line = lax.broadcasted_iota(jnp.int32, (lines, 1), 0)
    for g in range(groups):
        key, value = fresh[g]
        latest = jnp.sum(pairs[g] * key[:, None, :], axis=-1, keepdims=True) * scale
        masked = jnp.where(valid, scores[g], -jnp.inf)
        top = jnp.maximum(jnp.max(masked, axis=-1, keepdims=True), latest)
        raised = jnp.exp(masked - top)
        raised_new = jnp.exp(latest - top)
        total = jnp.sum(raised, axis=-1, keepdims=True) + raised_new
        prob = raised / total
        prob_new = jnp.broadcast_to(raised_new / total, (seqs, lines, LANES))
        lam = jnp.zeros((lines, 1), F32)
        for j in range(share):
            lam = jnp.where(line == j, lam_ref[g * share + j], lam)
        scores[g] = prob - lam[None] * pltpu.roll(prob, share, 1)
        new_weight = (prob_new - lam[None] * pltpu.roll(prob_new, share, 1)).astype(BF16).astype(F32)
        fresh_part = new_weight * value[:, None, :]
        for s in range(seqs):
            mixed[g, s] = dot(scores[g, s].astype(BF16), cache[s, g, :, LANES:])
        whole = mixed[g] + fresh_part
        mean_sq = jnp.mean(whole * whole, axis=-1, keepdims=True)
        mixed[g] = whole * lax.rsqrt(mean_sq + EPS) * head_gain_ref[...][None]
        for j in range(share):
            at = (g * share + j) * LANES
            heads_ref[:, at : at + LANES] = mixed[g, :, j, :].astype(BF16)

    def heads_copy(mask):
        return remote(
            heads_ref,
            heads_all.at[mask - 1],
            heads_send.at[mask - 1],
            heads_recv.at[mask - 1],
            (e, flip(t, mask)),
        )

    for mask in range(n_tp - 1, 0, -1):
        heads_copy(mask).start()

    loads[0].wait()
    span = heads_ref.shape[1]
    total = dot(heads_ref[...], ow[block(t, span), :])
    for mask in range(1, n_tp):
        heads_copy(mask).wait_recv()
        total = total + dot(heads_all[mask - 1], ow[block(flip(t, mask), span), :])
    own_cols = block(t, quarter)
    own_stream = (resid_ref[:, own_cols].astype(F32) + total).astype(BF16)
    stream[own_rows, own_cols] = own_stream

    def spot(owner, column):
        return stream.at[block(owner, seqs), block(column, quarter)]

    def owner_of(d):
        return (e + n_ep - d) % n_ep

    def first(d):
        return remote(
            spot(e, t), spot(e, t), first_send.at[d], stream_recv.at[0, d], ((e + d) % n_ep, t)
        )

    def second(d, mask):
        index = mask // 2 if mask != 1 else 0
        where = spot(owner_of(d), t)
        return remote(
            where, where, second_send.at[index, d], stream_recv.at[mask, d], (e, flip(t, mask))
        )

    def relay(d, mask):
        where = spot(owner_of(d), flip(t, mask))
        return remote(
            where, where, relay_send.at[mask // 2 - 1, d], stream_recv.at[mask + 1, d], (e, mate)
        )

    def arrived(d, mask):
        where = spot(owner_of(d), flip(t, mask))
        remote(where, where, first_send.at[d], stream_recv.at[mask, d], (e, t)).wait_recv()

    def spread(d):
        for mask in evens:
            second(d, mask).start()
        second(d, 1).start()

    far_first = sorted(range(1, n_ep), key=lambda d: -min(d, n_ep - d)) if n_ep <= 16 else None
    near_first = [0] + far_first[::-1] if far_first is not None else None
    each(n_ep - 1 if far_first is None else 1, lambda i: first(i + 1).start(), order=None) if far_first is None else [
        first(d).start() for d in far_first
    ]

    def stage_two(d):
        if not (isinstance(d, int) and d == 0):
            arrived(d, 0)
        spread(d)

    def stage_three(d):
        for mask in evens:
            arrived(d, mask)
            relay(d, mask).start()

    def normalise(d):
        arrived(d, 1)
        for mask in evens:
            arrived(d, mask + 1)
        rows = block(owner_of(d), seqs)
        values = stream[rows, :].astype(F32)
        mean_sq = jnp.mean(values * values, axis=-1, keepdims=True)
        scaled = (values * lax.rsqrt(mean_sq + EPS) * gain_ref[...]).astype(BF16)
        ffn[rows, :] = scaled
        inner = jnp.sum(scaled.astype(F32) * mixw_ref[...], axis=-1, keepdims=True)
        mix[rows, :] = jnp.broadcast_to(jax.nn.sigmoid(inner), (seqs, LANES))

    if near_first is not None:
        for i, d in enumerate(near_first):
            stage_two(d)
            if i:
                stage_three(near_first[i - 1])
            if i > 1:
                normalise(near_first[i - 2])
        stage_three(near_first[-1])
        for d in near_first[-2:]:
            normalise(d)
    else:
        stage_two(0)
        each(n_ep - 1, lambda i: stage_two(i + 1))
        each(n_ep, stage_three)
        each(n_ep, normalise)
    each(n_ep - 1, lambda i: route_wait(i + 1))

    many = min(rows_all, 128)
    batches = rows_all // many
    for load in loads[1:5]:
        load.wait()

    def hidden(b):
        rows = block(b, many)
        a = ffn[rows, :]
        for j in range(held):
            eh[j, rows, :] = (jax.nn.silu(dot(a, eg[j])) * dot(a, eu[j])).astype(BF16)
        units = jax.nn.silu(dot(a, dg[...])) * dot(a, du[...])
        if not split:
            own = hid // n_tp
            unit = lax.broadcasted_iota(jnp.int32, units.shape, 1)
            units = jnp.where((unit >= t * own) & (unit < (t + 1) * own), units, 0.0)
        dh[rows, :] = units.astype(BF16)

    each(batches, hidden)
    for load in loads[5:]:
        load.wait()

    def result(b, q):
        rows = block(b, many)
        cols = block(q, quarter)
        total = mix[rows, :1] * dot(dh[rows, :], dd[:, cols])
        lanes = lax.broadcasted_iota(jnp.int32, (many, route.shape[1]), 1)
        for j in range(held):
            weight = jnp.sum(
                jnp.where(lanes == e * held + j, route[rows, :], 0.0), axis=1, keepdims=True
            )
            piece = dot(eh[j, rows, :], ed[j, :, cols]).astype(BF16)
            total = total + weight * piece.astype(F32)
        return total

    def pair(j):
        return remote(away.at[j], came.at[j], pair_send.at[j], pair_recv.at[j], (e, mate))

    for j in range(half):

        def leave(b, j=j):
            away[j, block(b, many), :] = result(b, 2 * j + 1 - core).astype(BF16)

        each(batches, leave)
        pair(j).start()

    me = e * half + t // 2

    def back(j, d):
        there = (e + d) % n_ep
        return remote(
            summed.at[j, block(there, seqs), :],
            landed.at[me],
            back_send.at[j, d],
            back_recv.at[me],
            (there, 2 * j + core),
        )

    def same(j, d):
        return jnp.logical_and(jnp.asarray(d == 0), 2 * j + core == t)

    for j in range(half):

        def keep(b, j=j):
            summed[j, block(b, many), :] = result(b, 2 * j + core).astype(BF16)

        each(batches, keep)
    for j in range(half):
        pair(j).wait_recv()

        def add(b, j=j):
            rows = block(b, many)
            summed[j, rows, :] = (summed[j, rows, :].astype(F32) + came[j, rows, :].astype(F32)).astype(BF16)

        each(batches, add)

        def send(d, j=j):
            @pl.when(jnp.logical_not(same(j, d)))
            def _():
                back(j, d).start()

        each(n_ep, send, order=None if far_first is None else far_first + [0])

    landed[me] = summed[t // 2, own_rows, :]

    def take(index):
        @pl.when(index != me)
        def _():
            where = landed.at[index]
            remote(where, where, back_send.at[0, 0], back_recv.at[index], (e, t)).wait_recv()

    each(n_ep * half, take)
    out_ref[...] = own_stream.astype(F32) + jnp.sum(landed[...].astype(F32), axis=0)

    for mask in range(1, n_tp):
        heads_copy(mask).wait_send()
    each(n_ep - 1, lambda i: route_copy(i + 1).wait_send())
    each(n_ep - 1, lambda i: first(i + 1).wait_send())

    def sent(d):
        second(d, 1).wait_send()
        for mask in evens:
            second(d, mask).wait_send()
            relay(d, mask).wait_send()

    each(n_ep, sent)
    for j in range(half):
        pair(j).wait_send()

        def gone(d, j=j):
            @pl.when(jnp.logical_not(same(j, d)))
            def _():
                back(j, d).wait_send()

        each(n_ep, gone)


def on_device(
    residual_in,
    lengths,
    kv_cache,
    norm_gain_attn,
    query_weight,
    key_weight,
    value_weight,
    diff_lambda,
    head_gain,
    out_weight,
    norm_gain_ffn,
    route_ids,
    route_weights,
    expert_gate,
    expert_up,
    expert_down,
    dense_gate,
    dense_up,
    dense_down,
    dense_mix,
):
    n_ep = lax.axis_size("ep")
    n_tp = lax.axis_size("tp")
    half = n_tp // 2
    seqs, width = residual_in.shape
    groups, spots = kv_cache.shape[1:3]
    share = diff_lambda.shape[0] // groups
    inner = query_weight.shape[1]
    quarter = out_weight.shape[1]
    held, _, part = expert_gate.shape
    rows = n_ep * seqs
    own = dense_gate.shape[1] // n_tp
    split = own % LANES == 0
    hid = own if split else dense_gate.shape[1]
    lanes = -(-n_ep * held // LANES) * LANES
    vmem = pl.BlockSpec(memory_space=pltpu.VMEM)
    smem = pl.BlockSpec(memory_space=pltpu.SMEM)
    hbm = pl.BlockSpec(memory_space=pl.ANY)
    dma = pltpu.SemaphoreType.DMA
    layer_out, fresh = pl.pallas_call(
        functools.partial(layer_kernel, n_ep, n_tp, split),
        out_shape=(
            jax.ShapeDtypeStruct((seqs, quarter), F32),
            jax.ShapeDtypeStruct((seqs, groups * kv_cache.shape[3]), F32),
        ),
        in_specs=[smem] * 2 + [vmem] * 7 + [hbm] * 11,
        out_specs=(vmem, vmem),
        scratch_shapes=[
            pltpu.VMEM(query_weight.shape, BF16),
            pltpu.VMEM(key_weight.shape, BF16),
            pltpu.VMEM(value_weight.shape, BF16),
            pltpu.VMEM(kv_cache.shape, BF16),
            pltpu.VMEM((groups, seqs, 2 * share, LANES), F32),
            pltpu.VMEM((groups, seqs, 2 * share, spots), F32),
            pltpu.VMEM((groups, seqs, 2 * share, LANES), F32),
            pltpu.VMEM((seqs, inner), BF16),
            pltpu.VMEM(out_weight.shape, BF16),
            pltpu.VMEM(expert_gate.shape, BF16),
            pltpu.VMEM(expert_up.shape, BF16),
            pltpu.VMEM(expert_down.shape, BF16),
            pltpu.VMEM((width, hid), BF16),
            pltpu.VMEM((width, hid), BF16),
            pltpu.VMEM((hid, width), BF16),
            pltpu.VMEM((n_tp - 1, seqs, inner), BF16),
            pltpu.VMEM((rows, width), BF16),
            pltpu.VMEM((rows, width), BF16),
            pltpu.VMEM((rows, LANES), F32),
            pltpu.VMEM((rows, lanes), F32),
            pltpu.VMEM((held, rows, part), BF16),
            pltpu.VMEM((rows, hid), BF16),
            pltpu.VMEM((half, rows, quarter), BF16),
            pltpu.VMEM((half, rows, quarter), BF16),
            pltpu.VMEM((half, rows, quarter), BF16),
            pltpu.VMEM((n_ep * half, seqs, quarter), BF16),
            dma((7,)),
            dma((Q_CHUNKS + 2,)),
            dma((seqs,)),
            dma((n_ep - 1,)),
            dma((n_ep - 1,)),
            dma((n_tp - 1,)),
            dma((n_tp - 1,)),
            dma((n_ep,)),
            dma((half, n_ep)),
            dma((max(half - 1, 1), n_ep)),
            dma((n_tp, n_ep)),
            dma((half,)),
            dma((half,)),
            dma((half, n_ep)),
            dma((n_ep * half,)),
        ],
        compiler_params=pltpu.CompilerParams(
            collective_id=0, has_side_effects=True, vmem_limit_bytes=60 * 1024 * 1024
        ),
    )(
        lengths,
        diff_lambda,
        residual_in,
        norm_gain_attn[None, :],
        head_gain[None, :],
        norm_gain_ffn[None, :],
        dense_mix[None, :],
        route_ids.T,
        route_weights.T,
        query_weight,
        key_weight,
        value_weight,
        kv_cache,
        out_weight,
        expert_gate,
        expert_up,
        expert_down,
        dense_gate,
        dense_up,
        dense_down,
    )
    new_rows = fresh.astype(BF16).reshape(seqs, groups, kv_cache.shape[3])
    return (layer_out.astype(BF16), new_rows)


def solution(mesh):
    placed = (
        P("ep", None),
        P("ep"),
        P("ep", "tp", None, None),
        P(),
        P(None, "tp"),
        P(None, "tp"),
        P(None, "tp"),
        P("tp"),
        P(),
        P(None, "tp"),
        P(),
        P("ep", None),
        P("ep", None),
        P("ep", None, "tp"),
        P("ep", None, "tp"),
        P("ep", "tp", None),
        P(None, "ep"),
        P(None, "ep"),
        P("ep", None),
        P(),
    )
    return jax.shard_map(
        on_device,
        mesh=mesh,
        in_specs=placed,
        out_specs=(P("ep", "tp"), P("ep", "tp", None)),
        check_vma=False,
    )
```

```python
import functools
import math

import jax
import jax.numpy as jnp
from jax import lax
from jax.experimental import pallas as pl
from jax.experimental.pallas import tpu as pltpu
from jax.sharding import PartitionSpec as P

QK_DIM = 64
EPS = 1e-06
MESH = pl.DeviceIdType.MESH
F32 = jnp.float32
BF16 = jnp.bfloat16
LANES = 128
Q_CHUNKS = 4


def flip(value, mask):
    bit = 1
    while bit <= mask:
        if mask & bit:
            value = value + bit * (1 - 2 * ((value // bit) % 2))
        bit *= 2
    return value


def each(count, body, order=None):
    if count <= 16:
        for index in order if order is not None else range(count):
            body(index)
    else:

        def step(index, carry):
            body(index)
            return carry

        lax.fori_loop(0, count, step, 0)


def block(start, size):
    return pl.ds(pl.multiple_of(start * size, size), size)


def remote(source, target, send, recv, where):
    return pltpu.make_async_remote_copy(
        src_ref=source,
        dst_ref=target,
        send_sem=send,
        recv_sem=recv,
        device_id=where,
        device_id_type=MESH,
    )


def dot(left, right):
    return jnp.dot(left, right, preferred_element_type=F32)


def column(row):
    count = row.shape[1]
    square = (count, count)
    same = lax.broadcasted_iota(jnp.int32, square, 0) == lax.broadcasted_iota(jnp.int32, square, 1)
    return jnp.sum(jnp.where(same, row, jnp.zeros_like(row)), axis=1, keepdims=True)


def layer_kernel(
    n_ep,
    n_tp,
    split,
    lengths_ref,
    lam_ref,
    resid_ref,
    first_gain_ref,
    head_gain_ref,
    gain_ref,
    mixw_ref,
    ids_ref,
    rw_ref,
    qw_hbm,
    kw_hbm,
    vw_hbm,
    cache_hbm,
    ow_hbm,
    eg_hbm,
    eu_hbm,
    ed_hbm,
    dg_hbm,
    du_hbm,
    dd_hbm,
    out_ref,
    new_ref,
    qw,
    kw,
    vw,
    cache,
    pairs,
    scores,
    mixed,
    heads_ref,
    ow,
    eg,
    eu,
    ed,
    dg,
    du,
    dd,
    heads_all,
    stream,
    ffn,
    mix,
    route,
    eh,
    dh,
    away,
    came,
    summed,
    crossed,
    landed,
    w_sem,
    q_sem,
    cache_sem,
    route_send,
    route_recv,
    heads_send,
    heads_recv,
    first_send,
    second_send,
    relay_send,
    stream_recv,
    pair_send,
    pair_recv,
    cross_send,
    cross_recv,
    back_send,
    back_recv,
):
    e = lax.axis_index("ep")
    t = lax.axis_index("tp")
    half = n_tp // 2
    mate = flip(t, 1)
    seqs, width = resid_ref.shape
    quarter = out_ref.shape[1]
    held, _, part = eg.shape
    hid = dg.shape[1]
    rows_all = n_ep * seqs
    evens = [2 * i for i in range(1, half)]

    depth = qw.shape[0] // Q_CHUNKS
    q_loads = [
        pltpu.make_async_copy(
            qw_hbm.at[pl.ds(i * depth, depth), :], qw.at[pl.ds(i * depth, depth), :], q_sem.at[i]
        )
        for i in range(Q_CHUNKS)
    ] + [
        pltpu.make_async_copy(kw_hbm, kw, q_sem.at[Q_CHUNKS]),
        pltpu.make_async_copy(vw_hbm, vw, q_sem.at[Q_CHUNKS + 1]),
    ]
    for load in q_loads:
        load.start()
    cache_loads = [
        pltpu.make_async_copy(cache_hbm.at[s], cache.at[s], cache_sem.at[s]) for s in range(seqs)
    ]
    for load in cache_loads:
        load.start()

    barrier = pltpu.get_barrier_semaphore()

    def greet(index):
        pl.semaphore_signal(
            barrier, inc=1, device_id=((e + index + 1) % n_ep, t), device_id_type=MESH
        )

    each(n_ep - 1, greet)
    for mask in range(1, n_tp):
        pl.semaphore_signal(barrier, inc=1, device_id=(e, flip(t, mask)), device_id_type=MESH)

    if split:
        cols = block(t, hid)
        dense_parts = (dg_hbm.at[:, cols], du_hbm.at[:, cols], dd_hbm.at[cols, :])
    else:
        dense_parts = (dg_hbm, du_hbm, dd_hbm)
    loads = [
        pltpu.make_async_copy(src, dst, w_sem.at[i])
        for i, (src, dst) in enumerate(
            zip((ow_hbm, eg_hbm, eu_hbm) + dense_parts[:2] + (ed_hbm, dense_parts[2]), (ow, eg, eu, dg, du, ed, dd))
        )
    ]

    lane = lax.broadcasted_iota(jnp.int32, (seqs, route.shape[1]), 1)
    table = jnp.zeros((seqs, route.shape[1]), F32)
    for k in range(ids_ref.shape[0]):
        wanted = column(ids_ref[k : k + 1, :])
        table = table + jnp.where(lane == wanted, column(rw_ref[k : k + 1, :]), 0.0)
    own_rows = block(e, seqs)
    route[own_rows, :] = table

    resid = resid_ref[...].astype(F32)
    mean_sq = jnp.mean(resid * resid, axis=-1, keepdims=True)
    normed = (resid * lax.rsqrt(mean_sq + EPS) * first_gain_ref[...]).astype(BF16)
    row = lax.broadcasted_iota(jnp.int32, (seqs, LANES), 0)
    entry = lax.broadcasted_iota(jnp.int32, (seqs, LANES), 1) % QK_DIM
    position = jnp.zeros((seqs, LANES), F32)
    for s in range(seqs):
        position = jnp.where(row == s, lengths_ref[s].astype(F32), position)
    turn = QK_DIM // 2
    power = (entry % turn).astype(F32) * (-1.0 / turn)
    angle = position * jnp.exp(power * math.log(10000.0))
    cosine = jnp.cos(angle)
    sine = jnp.where(entry < turn, -jnp.sin(angle), jnp.sin(angle))

    def rotate(values):
        other = jnp.where(
            entry < turn, pltpu.roll(values, LANES - turn, 1), pltpu.roll(values, turn, 1)
        )
        return (values * cosine + other * sine).astype(BF16).astype(F32)

    query = jnp.zeros((seqs, qw.shape[1]), F32)
    for i in range(Q_CHUNKS):
        q_loads[i].wait()
        query = query + dot(
            normed[:, i * depth : (i + 1) * depth], qw[i * depth : (i + 1) * depth, :]
        )
    for load in q_loads[Q_CHUNKS:]:
        load.wait()
    keys_raw = dot(normed, kw[...])
    values_raw = dot(normed, vw[...])
    for load in loads:
        load.start()

    groups, spots = cache.shape[1], cache.shape[2]
    share = query.shape[1] // LANES // groups
    lower = lax.broadcasted_iota(jnp.int32, (seqs, LANES), 1) < QK_DIM
    fresh = []
    for g in range(groups):
        key = rotate(keys_raw[:, g * LANES : (g + 1) * LANES])
        value = values_raw[:, g * LANES : (g + 1) * LANES].astype(BF16).astype(F32)
        new_ref[:, 2 * g * LANES : (2 * g + 1) * LANES] = key
        new_ref[:, (2 * g + 1) * LANES : (2 * g + 2) * LANES] = value
        fresh.append((key, value))
        for j in range(share):
            at = (g * share + j) * LANES
            head = rotate(query[:, at : at + LANES])
            pairs[g, :, j, :] = jnp.where(lower, head, 0.0)
            pairs[g, :, share + j, :] = jnp.where(lower, 0.0, head)

    pl.semaphore_wait(barrier, n_ep + n_tp - 2)

    def route_copy(d):
        there = (e + d) % n_ep
        return remote(
            route.at[own_rows, :],
            route.at[own_rows, :],
            route_send.at[d - 1],
            route_recv.at[d - 1],
            (there, t),
        )

    def route_wait(d):
        came_from = (e + n_ep - d) % n_ep
        spot = route.at[block(came_from, seqs), :]
        remote(spot, spot, route_send.at[d - 1], route_recv.at[d - 1], (e, t)).wait_recv()

    each(n_ep - 1, lambda i: route_copy(i + 1).start())

    scale = QK_DIM**-0.5
    lines = 2 * share
    for s in range(seqs):
        cache_loads[s].wait()
        for g in range(groups):
            both = pairs[g, s].astype(BF16)
            scores[g, s] = (
                lax.dot_general(
                    both,
                    cache[s, g, :, :LANES],
                    (((1,), (1,)), ((), ())),
                    preferred_element_type=F32,
                )
                * scale
            )
    length = jnp.zeros((seqs, lines, 1), jnp.int32)
    which = lax.broadcasted_iota(jnp.int32, (seqs, lines, 1), 0)
    for s in range(seqs):
        length = jnp.where(which == s, lengths_ref[s], length)
    place = lax.broadcasted_iota(jnp.int32, (seqs, lines, spots), 2)
    valid = place < length
    line = lax.broadcasted_iota(jnp.int32, (lines, 1), 0)
    for g in range(groups):
        key, value = fresh[g]
        latest = jnp.sum(pairs[g] * key[:, None, :], axis=-1, keepdims=True) * scale
        masked = jnp.where(valid, scores[g], -jnp.inf)
        top = jnp.maximum(jnp.max(masked, axis=-1, keepdims=True), latest)
        raised = jnp.exp(masked - top)
        raised_new = jnp.exp(latest - top)
        total = jnp.sum(raised, axis=-1, keepdims=True) + raised_new
        prob = raised / total
        prob_new = jnp.broadcast_to(raised_new / total, (seqs, lines, LANES))
        lam = jnp.zeros((lines, 1), F32)
        for j in range(share):
            lam = jnp.where(line == j, lam_ref[g * share + j], lam)
        scores[g] = prob - lam[None] * pltpu.roll(prob, share, 1)
        new_weight = (prob_new - lam[None] * pltpu.roll(prob_new, share, 1)).astype(BF16).astype(F32)
        fresh_part = new_weight * value[:, None, :]
        for s in range(seqs):
            mixed[g, s] = dot(scores[g, s].astype(BF16), cache[s, g, :, LANES:])
        whole = mixed[g] + fresh_part
        mean_sq = jnp.mean(whole * whole, axis=-1, keepdims=True)
        mixed[g] = whole * lax.rsqrt(mean_sq + EPS) * head_gain_ref[...][None]
        for j in range(share):
            at = (g * share + j) * LANES
            heads_ref[:, at : at + LANES] = mixed[g, :, j, :].astype(BF16)

    def heads_copy(mask):
        return remote(
            heads_ref,
            heads_all.at[mask - 1],
            heads_send.at[mask - 1],
            heads_recv.at[mask - 1],
            (e, flip(t, mask)),
        )

    for mask in range(n_tp - 1, 0, -1):
        heads_copy(mask).start()

    loads[0].wait()
    span = heads_ref.shape[1]
    total = dot(heads_ref[...], ow[block(t, span), :])
    for mask in range(1, n_tp):
        heads_copy(mask).wait_recv()
        total = total + dot(heads_all[mask - 1], ow[block(flip(t, mask), span), :])
    own_cols = block(t, quarter)
    own_stream = (resid_ref[:, own_cols].astype(F32) + total).astype(BF16)
    stream[own_rows, own_cols] = own_stream

    def spot(owner, column):
        return stream.at[block(owner, seqs), block(column, quarter)]

    def owner_of(d):
        return (e + n_ep - d) % n_ep

    def first(d):
        return remote(
            spot(e, t), spot(e, t), first_send.at[d], stream_recv.at[0, d], ((e + d) % n_ep, t)
        )

    def second(d, mask):
        index = mask // 2 if mask != 1 else 0
        where = spot(owner_of(d), t)
        return remote(
            where, where, second_send.at[index, d], stream_recv.at[mask, d], (e, flip(t, mask))
        )

    def relay(d, mask):
        where = spot(owner_of(d), flip(t, mask))
        return remote(
            where, where, relay_send.at[mask // 2 - 1, d], stream_recv.at[mask + 1, d], (e, mate)
        )

    def arrived(d, mask):
        where = spot(owner_of(d), flip(t, mask))
        remote(where, where, first_send.at[d], stream_recv.at[mask, d], (e, t)).wait_recv()

    def spread(d):
        for mask in evens:
            second(d, mask).start()
        second(d, 1).start()

    far_first = sorted(range(1, n_ep), key=lambda d: -min(d, n_ep - d)) if n_ep <= 16 else None
    near_first = [0] + far_first[::-1] if far_first is not None else None
    each(n_ep - 1 if far_first is None else 1, lambda i: first(i + 1).start(), order=None) if far_first is None else [
        first(d).start() for d in far_first
    ]

    def stage_two(d):
        if not (isinstance(d, int) and d == 0):
            arrived(d, 0)
        spread(d)

    def stage_three(d):
        for mask in evens:
            arrived(d, mask)
            relay(d, mask).start()

    def normalise(d):
        arrived(d, 1)
        for mask in evens:
            arrived(d, mask + 1)
        rows = block(owner_of(d), seqs)
        values = stream[rows, :].astype(F32)
        mean_sq = jnp.mean(values * values, axis=-1, keepdims=True)
        scaled = (values * lax.rsqrt(mean_sq + EPS) * gain_ref[...]).astype(BF16)
        ffn[rows, :] = scaled
        inner = jnp.sum(scaled.astype(F32) * mixw_ref[...], axis=-1, keepdims=True)
        mix[rows, :] = jnp.broadcast_to(jax.nn.sigmoid(inner), (seqs, LANES))

    if near_first is not None:
        for i, d in enumerate(near_first):
            stage_two(d)
            if i:
                stage_three(near_first[i - 1])
            if i > 1:
                normalise(near_first[i - 2])
        stage_three(near_first[-1])
        for d in near_first[-2:]:
            normalise(d)
    else:
        stage_two(0)
        each(n_ep - 1, lambda i: stage_two(i + 1))
        each(n_ep, stage_three)
        each(n_ep, normalise)
    each(n_ep - 1, lambda i: route_wait(i + 1))

    many = min(rows_all, 128)
    batches = rows_all // many
    for load in loads[1:5]:
        load.wait()

    def hidden(b):
        rows = block(b, many)
        a = ffn[rows, :]
        for j in range(held):
            eh[j, rows, :] = (jax.nn.silu(dot(a, eg[j])) * dot(a, eu[j])).astype(BF16)
        units = jax.nn.silu(dot(a, dg[...])) * dot(a, du[...])
        if not split:
            own = hid // n_tp
            unit = lax.broadcasted_iota(jnp.int32, units.shape, 1)
            units = jnp.where((unit >= t * own) & (unit < (t + 1) * own), units, 0.0)
        dh[rows, :] = units.astype(BF16)

    each(batches, hidden)
    for load in loads[5:]:
        load.wait()

    def result(b, q):
        rows = block(b, many)
        cols = block(q, quarter)
        total = mix[rows, :1] * dot(dh[rows, :], dd[:, cols])
        lanes = lax.broadcasted_iota(jnp.int32, (many, route.shape[1]), 1)
        for j in range(held):
            weight = jnp.sum(
                jnp.where(lanes == e * held + j, route[rows, :], 0.0), axis=1, keepdims=True
            )
            piece = dot(eh[j, rows, :], ed[j, :, cols]).astype(BF16)
            total = total + weight * piece.astype(F32)
        return total

    def pair(j):
        return remote(away.at[j], came.at[j], pair_send.at[j], pair_recv.at[j], (e, mate))

    masks = evens + [0]
    for j, mask in enumerate(masks):

        def leave(b, j=j, mask=mask):
            away[j, block(b, many), :] = result(b, flip(mate, mask)).astype(BF16)

        each(batches, leave)
        pair(j).start()

    def cross(j, d):
        rows = block((e + d) % n_ep, seqs)
        return remote(
            summed.at[j, rows, :],
            crossed.at[j, rows, :],
            cross_send.at[j, d],
            cross_recv.at[j, d],
            (e, flip(t, masks[j])),
        )

    final = half - 1

    def back(d):
        there = (e + d) % n_ep
        return remote(
            summed.at[final, block(there, seqs), :],
            landed.at[d - 1],
            back_send.at[d - 1],
            back_recv.at[d - 1],
            (there, t),
        )

    for j, mask in enumerate(masks):
        if batches == 1:
            whole = result(0, flip(t, mask))
            pair(j).wait_recv()
            summed[j] = (whole + came[j].astype(F32)).astype(BF16)
        else:
            pair(j).wait_recv()

            def keep(b, j=j, mask=mask):
                rows = block(b, many)
                whole = result(b, flip(t, mask)) + came[j, rows, :].astype(F32)
                summed[j, rows, :] = whole.astype(BF16)

            each(batches, keep)
        if mask:
            each(
                n_ep,
                lambda d, j=j: cross(j, d).start(),
                order=None if far_first is None else far_first + [0],
            )

    def gathered(d):
        rows = block((e + d) % n_ep, seqs)
        whole = summed[final, rows, :].astype(F32)
        for j in range(final):
            cross(j, d).wait_recv()
            whole = whole + crossed[j, rows, :].astype(F32)
        return rows, whole

    def pass_on(i):
        d = i + 1
        rows, whole = gathered(d)
        summed[final, rows, :] = whole.astype(BF16)
        back(d).start()

    each(n_ep - 1, pass_on, order=None if far_first is None else [d - 1 for d in far_first])
    _, local = gathered(0)
    each(n_ep - 1, lambda i: back(i + 1).wait_recv())
    out_ref[...] = own_stream.astype(F32) + local + jnp.sum(landed[...].astype(F32), axis=0)

    for mask in range(1, n_tp):
        heads_copy(mask).wait_send()
    each(n_ep - 1, lambda i: route_copy(i + 1).wait_send())
    each(n_ep - 1, lambda i: first(i + 1).wait_send())

    def sent(d):
        second(d, 1).wait_send()
        for mask in evens:
            second(d, mask).wait_send()
            relay(d, mask).wait_send()

    each(n_ep, sent)
    for j in range(half):
        pair(j).wait_send()
    for j in range(final):
        each(n_ep, lambda d, j=j: cross(j, d).wait_send())
    each(n_ep - 1, lambda i: back(i + 1).wait_send())


def on_device(
    residual_in,
    lengths,
    kv_cache,
    norm_gain_attn,
    query_weight,
    key_weight,
    value_weight,
    diff_lambda,
    head_gain,
    out_weight,
    norm_gain_ffn,
    route_ids,
    route_weights,
    expert_gate,
    expert_up,
    expert_down,
    dense_gate,
    dense_up,
    dense_down,
    dense_mix,
):
    n_ep = lax.axis_size("ep")
    n_tp = lax.axis_size("tp")
    half = n_tp // 2
    seqs, width = residual_in.shape
    groups, spots = kv_cache.shape[1:3]
    share = diff_lambda.shape[0] // groups
    inner = query_weight.shape[1]
    quarter = out_weight.shape[1]
    held, _, part = expert_gate.shape
    rows = n_ep * seqs
    own = dense_gate.shape[1] // n_tp
    split = own % LANES == 0
    hid = own if split else dense_gate.shape[1]
    lanes = -(-n_ep * held // LANES) * LANES
    vmem = pl.BlockSpec(memory_space=pltpu.VMEM)
    smem = pl.BlockSpec(memory_space=pltpu.SMEM)
    hbm = pl.BlockSpec(memory_space=pltpu.HBM)
    dma = pltpu.SemaphoreType.DMA
    layer_out, fresh = pl.pallas_call(
        functools.partial(layer_kernel, n_ep, n_tp, split),
        out_shape=(
            jax.ShapeDtypeStruct((seqs, quarter), F32),
            jax.ShapeDtypeStruct((seqs, groups * kv_cache.shape[3]), F32),
        ),
        in_specs=[smem] * 2 + [vmem] * 7 + [hbm] * 11,
        out_specs=(vmem, vmem),
        scratch_shapes=[
            pltpu.VMEM(query_weight.shape, BF16),
            pltpu.VMEM(key_weight.shape, BF16),
            pltpu.VMEM(value_weight.shape, BF16),
            pltpu.VMEM(kv_cache.shape, BF16),
            pltpu.VMEM((groups, seqs, 2 * share, LANES), F32),
            pltpu.VMEM((groups, seqs, 2 * share, spots), F32),
            pltpu.VMEM((groups, seqs, 2 * share, LANES), F32),
            pltpu.VMEM((seqs, inner), BF16),
            pltpu.VMEM(out_weight.shape, BF16),
            pltpu.VMEM(expert_gate.shape, BF16),
            pltpu.VMEM(expert_up.shape, BF16),
            pltpu.VMEM(expert_down.shape, BF16),
            pltpu.VMEM((width, hid), BF16),
            pltpu.VMEM((width, hid), BF16),
            pltpu.VMEM((hid, width), BF16),
            pltpu.VMEM((n_tp - 1, seqs, inner), BF16),
            pltpu.VMEM((rows, width), BF16),
            pltpu.VMEM((rows, width), BF16),
            pltpu.VMEM((rows, LANES), F32),
            pltpu.VMEM((rows, lanes), F32),
            pltpu.VMEM((held, rows, part), BF16),
            pltpu.VMEM((rows, hid), BF16),
            pltpu.VMEM((half, rows, quarter), BF16),
            pltpu.VMEM((half, rows, quarter), BF16),
            pltpu.VMEM((half, rows, quarter), BF16),
            pltpu.VMEM((max(half - 1, 1), rows, quarter), BF16),
            pltpu.VMEM((n_ep - 1, seqs, quarter), BF16),
            dma((7,)),
            dma((Q_CHUNKS + 2,)),
            dma((seqs,)),
            dma((n_ep - 1,)),
            dma((n_ep - 1,)),
            dma((n_tp - 1,)),
            dma((n_tp - 1,)),
            dma((n_ep,)),
            dma((half, n_ep)),
            dma((max(half - 1, 1), n_ep)),
            dma((n_tp, n_ep)),
            dma((half,)),
            dma((half,)),
            dma((max(half - 1, 1), n_ep)),
            dma((max(half - 1, 1), n_ep)),
            dma((n_ep - 1,)),
            dma((n_ep - 1,)),
        ],
        compiler_params=pltpu.CompilerParams(
            collective_id=0, has_side_effects=True, vmem_limit_bytes=60 * 1024 * 1024
        ),
    )(
        lengths,
        diff_lambda,
        residual_in,
        norm_gain_attn[None, :],
        head_gain[None, :],
        norm_gain_ffn[None, :],
        dense_mix[None, :],
        route_ids.T,
        route_weights.T,
        query_weight,
        key_weight,
        value_weight,
        kv_cache,
        out_weight,
        expert_gate,
        expert_up,
        expert_down,
        dense_gate,
        dense_up,
        dense_down,
    )
    new_rows = fresh.astype(BF16).reshape(seqs, groups, kv_cache.shape[3])
    return (layer_out.astype(BF16), new_rows)


def solution(mesh):
    placed = (
        P("ep", None),
        P("ep"),
        P("ep", "tp", None, None),
        P(),
        P(None, "tp"),
        P(None, "tp"),
        P(None, "tp"),
        P("tp"),
        P(),
        P(None, "tp"),
        P(),
        P("ep", None),
        P("ep", None),
        P("ep", None, "tp"),
        P("ep", None, "tp"),
        P("ep", "tp", None),
        P(None, "ep"),
        P(None, "ep"),
        P("ep", None),
        P(),
    )
    return jax.shard_map(
        on_device,
        mesh=mesh,
        in_specs=placed,
        out_specs=(P("ep", "tp"), P("ep", "tp", None)),
        check_vma=False,
    )
```
